32 devices in a mesh: kv: 4 (over y, x), tp: 8 (over z, core).
Axes of the slice: x: 2, y: 2, z: 4, core: 2. Of those that a mesh axis runs over, the one named last changes fastest.
Arguments:
- tokens: bfloat16 [32, 4096], P(None, ('kv', 'tp')), may hold values from -60 to 60, as said below
- gain_mix: float32 [4096], replicated, may hold values from 0.1 to 1.9
- w_query: bfloat16 [4096, 4096], P('kv', 'tp'), may hold values from -0.09375 to 0.09375
- w_key: bfloat16 [4096, 4096], P('kv', 'tp'), may hold values from -0.75 to 0.75
- w_value: bfloat16 [4096, 4096], P('kv', 'tp'), may hold values from -0.09375 to 0.09375
- w_outgate: bfloat16 [4096, 4096], P('kv', 'tp'), may hold values from -0.09375 to 0.09375
- w_gates: bfloat16 [4096, 32], P('kv'), may hold values from -0.09375 to 0.09375
- forget_bias: float32 [16], replicated, may hold values from 0 to 4
- cell_state: float32 [32, 4096, 256], P('kv', 'tp'), may hold values from -1.5 to 1.5
- norm_state: float32 [32, 16, 256], P('kv'), may hold values from -1.5 to 1.5
- max_state: float32 [32, 16], P('kv'), may hold values from -1 to 2
- gain_group: float32 [4096], replicated, may hold values from 0.1 to 1.9
- w_mix: bfloat16 [4096, 4096], P('tp', 'kv'), may hold values from -0.125 to 0.125
- gain_ffn: float32 [4096], replicated, may hold values from 0.1 to 1.9
- w_up: bfloat16 [4096, 16384], P('kv', 'tp'), may hold values from -0.09375 to 0.09375
- w_down: bfloat16 [16384, 4096], P('tp', 'kv'), may hold values from -0.0625 to 0.0625
Outputs:
- layer_out: bfloat16 [32, 4096], P(None, ('kv', 'tp'))
- cell_next: float32 [32, 4096, 256], P('kv', 'tp')
- norm_next: float32 [32, 16, 256], P('kv')
- max_next: float32 [32, 16], P('kv')
The draws below stay inside these ranges and needn't reach their ends.
Inputs may be any that keep to these rules, and one draw needn't show every extreme that they name: `tokens`: finite activations.
All inputs are finite; a program needn't handle non-finite values.
Results may differ from the reference program's by a relative error of at most 0.019.
Values may be sent and summed in bfloat16 or wider, within the bound.
A program may use at most 64 MiB of HBM per device.

```python
import math
import jax
import jax.numpy as jnp
from jax import lax

D = 4096
HEADS = 16
HEAD_DIM = 256
FF = 16384
BATCH = 32


def draw_tokens(key, part):
    first = jax.random.fold_in(jax.random.fold_in(key, 11), 0)
    columns = jnp.arange(D, dtype=jnp.float32) / D
    base = jnp.clip(jax.random.normal(first, (BATCH, D), jnp.float32), -6.0, 6.0)
    col_scale = 0.3 * jnp.exp(columns * math.log(10.0))
    values = base * col_scale
    return values.astype(jnp.bfloat16)


def with_spikes(result, stream_key, source, target, blocks, factor):
    owner, partner = [(jnp.arange(result.shape[axis_at]) // (result.shape[axis_at] // blocks)).reshape([-1 if axis == axis_at else 1 for axis in range(result.ndim)]) for axis_at in (source, target)]
    chosen = jax.random.permutation(stream_key, blocks)[partner]
    strong = (owner == chosen) | (owner == (partner + blocks // 2) % blocks)
    return jnp.where(strong, factor * result, result)


def level_of(own_key, extent, shards, least, top_value):
    def one(position, parts):
        draws = jax.random.uniform(jax.random.fold_in(jax.random.fold_in(own_key, 6), position), (parts,), jnp.float32, least / len(shards), top_value / len(shards))
        return jnp.repeat(jnp.exp(draws), extent[position] // parts).reshape((-1,) + (1,) * (len(extent) - position - 1))

    gain = one(*shards[0])
    for cut in shards[1:]:
        gain = gain * one(*cut)
    return gain


def bell_draw(own_key, shape, scale, bound, cuts=(), kind=jnp.bfloat16):
    entries = jax.random.normal(own_key, shape, jnp.float32) * scale
    if len(cuts) > 0:
        entries = level_of(own_key, shape, cuts, -0.22, 0.18) * entries
    return jnp.clip(entries, min=-bound, max=bound).astype(kind)


def bell_draw_with(stream_key, extent, scale, bound, cuts, heavy, kind=jnp.bfloat16):
    array = scale * jax.random.normal(stream_key, extent, jnp.float32)
    if cuts:
        array = array * level_of(stream_key, extent, cuts, -0.22, 0.18)
    return jnp.clip(with_spikes(array, jax.random.fold_in(stream_key, 3), *heavy), -bound, bound).astype(kind)


def setup_inputs(seed: int = 0) -> dict:
    key_list = jax.random.split(jax.random.key(seed), 17)
    return {
        "tokens": draw_tokens(jax.random.fold_in(key_list[16], 71), 0),
        "gain_mix": jnp.clip(1.0 + 0.18 * jax.random.normal(key_list[1], (D,), jnp.float32), 0.1, 1.9),
        "w_query": bell_draw(key_list[2], (D, HEADS * HEAD_DIM), D ** -0.5, 0.09375, ((0, 4), (1, 8))),
        "w_key": bell_draw(key_list[3], (D, HEADS * HEAD_DIM), (D // 64) ** -0.5, 0.75, ((0, 4), (1, 8))),
        "w_value": bell_draw(key_list[4], (D, HEADS * HEAD_DIM), D ** -0.5, 0.09375, ((0, 4), (1, 8))),
        "w_outgate": bell_draw(key_list[5], (D, HEADS * HEAD_DIM), D ** -0.5, 0.09375, ((0, 4), (1, 8))),
        "w_gates": bell_draw(key_list[6], (D, 2 * HEADS), D ** -0.5, 0.09375, ((0, 4),)),
        "forget_bias": jnp.clip(jax.random.uniform(key_list[7], (HEADS,), jnp.float32, 0.0, 4.0), 0.0, 4.0),
        "cell_state": bell_draw(key_list[8], (BATCH, HEADS * HEAD_DIM, HEAD_DIM), 0.25, 1.5, ((0, 4), (1, 8)), jnp.float32),
        "norm_state": bell_draw(key_list[9], (BATCH, HEADS, HEAD_DIM), 0.25, 1.5, ((0, 4),), jnp.float32),
        "max_state": jnp.clip(-1.0 + 3.0 * jax.random.uniform(key_list[10], (BATCH, HEADS), jnp.float32) ** level_of(key_list[10], (BATCH, HEADS), ((0, 4),), -0.2, 0.2), -1.0, 2.0),
        "gain_group": jnp.clip(1.0 + 0.18 * jax.random.normal(key_list[11], (HEADS * HEAD_DIM,), jnp.float32), 0.1, 1.9),
        "w_mix": bell_draw_with(key_list[12], (HEADS * HEAD_DIM, D), (HEADS * HEAD_DIM) ** -0.5, 0.125, ((0, 8), (1, 4)), (0, 1, 8, 2.0)),
        "gain_ffn": jnp.clip(1.0 + 0.18 * jax.random.normal(key_list[13], (D,), jnp.float32), 0.1, 1.9),
        "w_up": bell_draw(key_list[14], (D, FF), D ** -0.5, 0.09375, ((0, 4), (1, 8))),
        "w_down": bell_draw_with(key_list[15], (FF, D), FF ** -0.5, 0.0625, ((0, 8), (1, 4)), (0, 1, 8, 2.0)),
    }


EPSILON = 1e-06

def reference(tokens, gain_mix, w_query, w_key, w_value, w_outgate, w_gates, forget_bias, cell_state, norm_state, max_state, gain_group, w_mix, gain_ffn, w_up, w_down):
    f32 = jnp.float32
    bf16 = jnp.bfloat16
    batch = tokens.shape[0]
    xf = tokens.astype(f32)
    scale_in = lax.rsqrt(lax.optimization_barrier(jnp.mean(xf * xf, axis=1, keepdims=True)) + EPSILON)
    normed = (xf * gain_mix).astype(bf16)
    query = (jnp.dot(normed, w_query, preferred_element_type=f32) * scale_in).astype(bf16)
    keys = (jnp.dot(normed, w_key, preferred_element_type=f32) * scale_in).astype(bf16)
    values = jnp.dot(normed, w_value, preferred_element_type=f32) * scale_in
    gate_out = jnp.dot(normed, w_outgate, preferred_element_type=f32) * scale_in
    gates = jnp.dot(normed, w_gates, preferred_element_type=f32) * scale_in
    gate_in = gates[:, :HEADS]
    log_forget = jax.nn.log_sigmoid(gates[:, HEADS:] + forget_bias)
    max_next = jnp.maximum(log_forget + max_state, gate_in)
    decay = jnp.exp(log_forget + max_state - max_next)
    inflow = jnp.exp(gate_in - max_next)
    qf = query.astype(f32).reshape(batch, HEADS, HEAD_DIM)
    kf = keys.astype(f32).reshape(batch, HEADS, HEAD_DIM) / math.sqrt(HEAD_DIM)
    vh = values.reshape(batch, HEADS, HEAD_DIM)
    cells = cell_state.reshape(batch, HEADS, HEAD_DIM, HEAD_DIM)
    cell_next = decay[..., None, None] * cells + inflow[..., None, None] * vh[..., :, None] * kf[..., None, :]
    norm_next = decay[..., None] * norm_state + inflow[..., None] * kf
    numer = jnp.einsum('bhvk,bhk->bhv', cell_next, qf, precision=lax.Precision.HIGHEST)
    denom = jnp.maximum(jnp.abs(lax.optimization_barrier(jnp.sum(norm_next * qf, axis=-1))), 1.0)
    cell_read = (jax.nn.sigmoid(gate_out) * (numer / denom[..., None]).reshape(batch, HEADS * HEAD_DIM)).astype(bf16)
    readf = cell_read.astype(f32)
    scale_group = lax.rsqrt(lax.optimization_barrier(jnp.mean(readf * readf, axis=1, keepdims=True)) + EPSILON)
    grouped = (readf * gain_group).astype(bf16)
    mixed = (xf + jnp.dot(grouped, w_mix, preferred_element_type=f32) * scale_group).astype(bf16)
    mixf = mixed.astype(f32)
    scale_ffn = lax.rsqrt(lax.optimization_barrier(jnp.mean(mixf * mixf, axis=1, keepdims=True)) + EPSILON)
    normed_ffn = (mixf * gain_ffn).astype(bf16)
    hidden = jnp.square(jax.nn.relu(jnp.dot(normed_ffn, w_up, preferred_element_type=f32) * scale_ffn)).astype(bf16)
    layer_out = (mixf + jnp.dot(hidden, w_down, preferred_element_type=f32)).astype(bf16)
    return (layer_out, cell_next.reshape(batch, HEADS * HEAD_DIM, HEAD_DIM), norm_next, max_next)
```

```python
import functools
import math

import jax
import jax.numpy as jnp
from jax import lax
from jax.experimental import pallas as pl
from jax.experimental.pallas import tpu as pltpu
from jax.sharding import PartitionSpec as P

EPSILON = 1e-06


def per_device(
    tokens,
    gain_mix,
    w_query,
    w_key,
    w_value,
    w_outgate,
    w_gates,
    forget_bias,
    cell_state,
    norm_state,
    max_state,
    gain_group,
    w_mix,
    gain_ffn,
    w_up,
    w_down,
):
    f32 = jnp.float32
    bf16 = jnp.bfloat16
    exact = lax.Precision.HIGHEST
    width = gain_mix.shape[0]
    kv_index = lax.axis_index("kv")
    tp_index = lax.axis_index("tp")
    tokf = tokens.astype(f32)
    block_rows = lax.all_gather(tokens, "tp", axis=1, tiled=True)
    block = block_rows.shape[1]
    blockf = block_rows.astype(f32)
    gain_block = lax.dynamic_slice_in_dim(gain_mix, kv_index * block, block)
    normed = (blockf * gain_block).astype(bf16)
    partials = tuple(
        (
            jnp.dot(normed, weight, preferred_element_type=f32)
            for weight in (w_query, w_key, w_value, w_outgate, w_gates)
        )
    )
    partials = partials + (jnp.sum(blockf * blockf, axis=1),)
    summed = lax.psum_scatter(partials, "kv", scatter_dimension=0, tiled=True)
    seqs = summed[0].shape[0]
    seq_squares = summed[5]
    scale_in = lax.rsqrt(seq_squares / width + EPSILON)[:, None]
    query_part = (summed[0] * scale_in).astype(bf16)
    key_part = (summed[1] * scale_in).astype(bf16)
    values = summed[2] * scale_in
    gate_out = summed[3] * scale_in
    gates = summed[4] * scale_in
    query_all, key_all = (
        lax.all_gather(query_part, "tp", axis=1, tiled=True),
        lax.all_gather(key_part, "tp", axis=1, tiled=True),
    )
    heads = forget_bias.shape[0]
    head_dim = cell_state.shape[2]
    value_rows = cell_state.shape[1]
    queryf = query_all.astype(f32).reshape(seqs, heads, head_dim)
    keyf = key_all.astype(f32).reshape(seqs, heads, head_dim) / math.sqrt(head_dim)
    gate_in = gates[:, :heads]
    log_forget = jax.nn.log_sigmoid(gates[:, heads:] + forget_bias)
    max_next = jnp.maximum(log_forget + max_state, gate_in)
    decay = jnp.exp(log_forget + max_state - max_next)
    inflow = jnp.exp(gate_in - max_next)
    norm_next = decay[..., None] * norm_state + inflow[..., None] * keyf
    denom_heads = jnp.maximum(jnp.abs(jnp.sum(norm_next * queryf, axis=2)), 1.0)
    row_ids = tp_index * value_rows + jnp.arange(value_rows)
    select = (row_ids[:, None] // head_dim == jnp.arange(heads)[None, :]).astype(f32)
    query_rows = jnp.einsum("shd,rh->srd", queryf, select, precision=exact)
    key_rows = jnp.einsum("shd,rh->srd", keyf, select, precision=exact)
    decay_rows = jnp.einsum("sh,rh->sr", decay, select, precision=exact)
    inflow_rows = jnp.einsum("sh,rh->sr", inflow, select, precision=exact)
    denom_rows = jnp.einsum("sh,rh->sr", denom_heads, select, precision=exact)
    cell_next = (
        decay_rows[:, :, None] * cell_state
        + inflow_rows[:, :, None] * values[:, :, None] * key_rows
    )
    numer = jnp.sum(cell_next * query_rows, axis=2)
    cell_read = (jax.nn.sigmoid(gate_out) * (numer / denom_rows)).astype(bf16)
    read_rows = lax.all_gather(cell_read, "kv", axis=0, tiled=True)
    readf = read_rows.astype(f32)
    group_total = lax.psum(jnp.sum(readf * readf, axis=1), "tp")
    scale_group = lax.rsqrt(group_total / (heads * head_dim) + EPSILON)[:, None]
    gain_rows = lax.dynamic_slice_in_dim(gain_group, tp_index * value_rows, value_rows)
    grouped = (readf * gain_rows).astype(bf16)
    mix_terms = jnp.dot(grouped, w_mix, preferred_element_type=f32)
    mix_summed = lax.psum_scatter(mix_terms, "tp", scatter_dimension=1, tiled=True)
    mixed = (tokf + mix_summed * scale_group).astype(bf16)
    ffn_block = w_up.shape[0]
    piece = lax.all_gather(mixed, "tp", axis=1, tiled=True)
    count = piece.shape[1]
    piecef = piece.astype(f32)
    gain_piece = lax.dynamic_slice_in_dim(gain_ffn, kv_index * ffn_block, count)
    normed_piece = (piecef * gain_piece).astype(bf16)
    up_part = jnp.dot(normed_piece, w_up, preferred_element_type=f32)
    square_part = jnp.sum(piecef * piecef, axis=1)
    up_total, square_total = lax.psum((up_part, square_part), "kv")
    scale_ffn = lax.rsqrt(square_total / width + EPSILON)[:, None]
    hidden = jnp.square(jax.nn.relu(up_total * scale_ffn)).astype(bf16)
    down_terms = jnp.dot(hidden, w_down, preferred_element_type=f32)
    ffn_summed = lax.psum_scatter(down_terms, "tp", scatter_dimension=1, tiled=True)
    layer_out = (mixed.astype(f32) + ffn_summed).astype(bf16)
    return (layer_out, cell_next, norm_next, max_next)


MESH = pl.DeviceIdType.MESH
LANES = 128
SUBLANES = 8
CHUNKS = 2


def stack_rows(ref, count):
    f32 = jnp.float32
    rows = [ref[j].astype(f32) for j in range(count)]
    return jnp.concatenate(rows, axis=0)


def fused_kernel(
    nk,
    nt,
    heads,
    head_dim,
    width,
    tokens,
    gain_mix,
    w_query,
    w_key,
    w_value,
    w_outgate,
    w_gates,
    forget_bias,
    cell_state,
    norm_state,
    max_state,
    gain_group,
    w_mix,
    gain_ffn,
    w_up,
    w_down,
    layer_out,
    rows_out,
    gates_out,
    keys_out,
    tok_v,
    gmix_v,
    wq_v,
    wk_v,
    wv_v,
    wo_v,
    wg_v,
    bias_v,
    cell_v,
    norm_v,
    max_v,
    ggroup_v,
    wmix_v,
    gffn_v,
    wup_v,
    wdown_v,
    cell_b,
    proj_part,
    proj_recv,
    gate_part,
    gate_recv,
    read_buf,
    sq_part,
    sq_recv,
    mix_part,
    mix_recv,
    mixed_buf,
    fsq_part,
    fsq_recv,
    up_part,
    up_recv,
    hid_buf,
    down_part,
    down_recv,
    local_sem,
    send_sem,
    recv_sem,
):
    f32 = jnp.float32
    bf16 = jnp.bfloat16
    kv = lax.axis_index("kv")
    tp = lax.axis_index("tp")
    batch, cols = tokens.shape
    seqs = batch // nk
    block = cols * nt
    vrows = wq_v.shape[1]
    own_heads = vrows // head_dim
    ffl = wup_v.shape[1]
    chunk = ffl // CHUNKS

    loads = {}

    def load(name, source, target):
        copy = pltpu.make_async_copy(source, target, local_sem.at[len(loads)])
        copy.start()
        loads[name] = copy

    load("tok", tokens, tok_v.at[tp])
    load("gmix", gain_mix, gmix_v)
    load("wq", w_query, wq_v)
    load("wk", w_key, wk_v)
    load("wv", w_value, wv_v)
    load("wo", w_outgate, wo_v)
    load("wg", w_gates, wg_v)

    barrier = pltpu.get_barrier_semaphore()
    for d in range(1, nt):
        pl.semaphore_signal(
            barrier, inc=1, device_id={"tp": lax.rem(tp + d, nt)}, device_id_type=MESH
        )
    for d in range(1, nk):
        pl.semaphore_signal(
            barrier, inc=1, device_id={"kv": lax.rem(kv + d, nk)}, device_id_type=MESH
        )
    pl.semaphore_wait(barrier, nt + nk - 2)

    used = [0]
    sent = []

    def exchange(axis, count, me, source, target):
        copies = []
        for d in range(1, count):
            peer = lax.rem(me + d, count)
            copy = pltpu.make_async_remote_copy(
                src_ref=source(peer),
                dst_ref=target,
                send_sem=send_sem.at[used[0]],
                recv_sem=recv_sem.at[used[0]],
                device_id={axis: peer},
                device_id_type=MESH,
            )
            copy.start()
            used[0] += 1
            copies.append(copy)
        sent.extend(copies)
        return copies

    def arrive(copies):
        for copy in copies:
            copy.wait_recv()

    def total(own, recv, me, count):
        result = own[me].astype(f32)
        for d in range(1, count):
            result = result + recv[lax.rem(me + count - d, count)].astype(f32)
        return result

    got = exchange("tp", nt, tp, lambda peer: tokens, tok_v.at[tp])
    load("cell", cell_state, cell_v)
    load("norm", norm_state, norm_v)
    load("max", max_state, max_v)
    load("bias", forget_bias, bias_v)
    load("ggroup", gain_group, ggroup_v)
    load("gffn", gain_ffn, gffn_v)
    load("wmix", w_mix, wmix_v)
    load("wup", w_up, wup_v)
    load("wdown", w_down, wdown_v)
    loads["tok"].wait()
    loads["gmix"].wait()
    arrive(got)
    blockf = jnp.concatenate([tok_v[j].astype(f32) for j in range(nt)], axis=1)
    gain = gmix_v[:, pl.ds(pl.multiple_of(kv * block, LANES), block)]
    normed = (blockf * gain).astype(bf16)
    squares = jnp.sum(blockf * blockf, axis=1, keepdims=True)
    loads["wg"].wait()
    gates_p = lax.dot_general(
        normed, wg_v[...], (((1,), (1,)), ((), ())), preferred_element_type=f32
    )
    squares_b = jnp.broadcast_to(squares, (batch, LANES))
    for j in range(nk):
        gate_part[j] = squares_b[j * seqs : (j + 1) * seqs]
        gate_part[j, :, : 2 * heads] = gates_p[j * seqs : (j + 1) * seqs]
    got_gates = exchange("kv", nk, kv, lambda peer: gate_part.at[peer], gate_recv.at[kv])
    got_proj = []
    for i, (name, weight) in enumerate((("wq", wq_v), ("wk", wk_v), ("wv", wv_v), ("wo", wo_v))):
        loads[name].wait()
        part = jnp.dot(normed, weight[...], preferred_element_type=f32)
        for j in range(nk):
            proj_part[i, j] = part[j * seqs : (j + 1) * seqs].astype(bf16)
        got_proj.append(
            exchange("kv", nk, kv, lambda peer, i=i: proj_part.at[i, peer], proj_recv.at[i, kv])
        )

    loads["cell"].wait()
    for s in range(seqs):
        cell_b[s] = cell_v[s].astype(bf16)
    loads["norm"].wait()
    loads["max"].wait()
    loads["bias"].wait()

    arrive(got_gates)
    gsum = total(gate_part, gate_recv, kv, nk)
    scale_in = lax.rsqrt(gsum[:, 2 * heads : 2 * heads + 1] / width + EPSILON)
    scaled = gsum * scale_in
    gate_in = scaled[:, :heads]
    gate_forget = pltpu.roll(scaled, LANES - heads, 1)[:, :heads]
    max_state_ = max_v[...]
    log_forget = jax.nn.log_sigmoid(gate_forget + bias_v[...])
    max_next = jnp.maximum(log_forget + max_state_, gate_in)
    decay = jnp.exp(log_forget + max_state_ - max_next)
    inflow = jnp.exp(gate_in - max_next)
    gates_out[0] = max_next
    gates_out[1] = decay
    gates_out[2] = inflow
    head_ids = lax.broadcasted_iota(jnp.int32, (seqs, heads), 1)

    def own(values, h):
        mine = jnp.where(head_ids == tp * own_heads + h, values, 0.0)
        return jnp.sum(mine, axis=1, keepdims=True)

    own_decay = [own(decay, h) for h in range(own_heads)]
    own_inflow = [own(inflow, h) for h in range(own_heads)]
    norm_ids = lax.broadcasted_iota(jnp.int32, (seqs, heads, head_dim), 1)
    norm_own = [
        jnp.sum(jnp.where(norm_ids == tp * own_heads + h, norm_v[...], 0.0), axis=1)
        for h in range(own_heads)
    ]

    sums = []
    for i in range(4):
        arrive(got_proj[i])
        sums.append(total(proj_part.at[i], proj_recv.at[i], kv, nk) * scale_in)
    query = sums[0].astype(bf16)
    key = sums[1].astype(bf16)
    values = sums[2]
    opened = jax.nn.sigmoid(sums[3])
    keys_out[tp] = key
    queryf = query.astype(f32)
    keyf = key.astype(f32) / math.sqrt(head_dim)
    row_ids = lax.broadcasted_iota(jnp.int32, (seqs, head_dim), 0)
    reads = []
    for h in range(own_heads):
        span = slice(h * head_dim, (h + 1) * head_dim)
        qh = queryf[:, span]
        kh = keyf[:, span]
        numer = jnp.zeros((seqs, head_dim), f32)
        for s in range(seqs):
            lhs = jnp.where(row_ids == s, qh, 0.0).astype(bf16)
            numer += lax.dot_general(
                lhs,
                cell_b[s, span, :],
                (((1,), (1,)), ((), ())),
                preferred_element_type=f32,
            )
        gain_k = own_inflow[h] * kh
        norm_h = own_decay[h] * norm_own[h] + gain_k
        denom = jnp.maximum(jnp.abs(jnp.sum(norm_h * qh, axis=1, keepdims=True)), 1.0)
        kq = jnp.sum(gain_k * qh, axis=1, keepdims=True)
        numer = own_decay[h] * numer + values[:, span] * kq
        reads.append((opened[:, span] * (numer / denom)).astype(bf16))
        rows_out[0, :, span] = values[:, span]
        rows_out[1, :, span] = gain_k
        rows_out[2, :, span] = jnp.broadcast_to(own_decay[h], (seqs, head_dim))
    read_buf[kv] = jnp.concatenate(reads, axis=1)
    got = exchange("kv", nk, kv, lambda peer: read_buf.at[kv], read_buf.at[kv])
    got_keys = exchange("tp", nt, tp, lambda peer: keys_out.at[tp], keys_out.at[tp])
    loads["ggroup"].wait()
    loads["wmix"].wait()
    gain = ggroup_v[:, pl.ds(pl.multiple_of(tp * vrows, LANES), vrows)]
    arrive(got)
    readf = stack_rows(read_buf, nk)
    groups = batch // SUBLANES
    stride = LANES // groups
    squares = jnp.sum(readf * readf, axis=1, keepdims=True)
    lane_ids = lax.broadcasted_iota(jnp.int32, (SUBLANES, LANES), 1)
    packed = jnp.zeros((SUBLANES, LANES), f32)
    for a in range(groups):
        packed = jnp.where(
            lane_ids // stride == a, squares[a * SUBLANES : (a + 1) * SUBLANES], packed
        )
    sq_part[...] = packed
    got_sq = exchange("tp", nt, tp, lambda peer: sq_part, sq_recv.at[tp])
    grouped = (readf * gain).astype(bf16)
    terms = jnp.dot(grouped, wmix_v[...], preferred_element_type=f32)
    for j in range(nt):
        mix_part[j] = terms[:, j * cols : (j + 1) * cols].astype(bf16)
    got = exchange("tp", nt, tp, lambda peer: mix_part.at[peer], mix_recv.at[tp])
    tokf = tok_v[tp].astype(f32)
    arrive(got_sq)
    for d in range(1, nt):
        packed = packed + sq_recv[lax.rem(tp + nt - d, nt)]
    scale_packed = lax.rsqrt(packed / (heads * head_dim) + EPSILON)
    scale_group = jnp.concatenate(
        [scale_packed[:, a * stride : a * stride + 1] for a in range(groups)], axis=0
    )
    arrive(got)
    mixed = (tokf + total(mix_part, mix_recv, tp, nt) * scale_group).astype(bf16)
    mixed_buf[tp] = mixed
    got = exchange("tp", nt, tp, lambda peer: mixed_buf.at[tp], mixed_buf.at[tp])
    loads["gffn"].wait()
    loads["wup"].wait()
    gain = gffn_v[:, pl.ds(pl.multiple_of(kv * block, LANES), block)]
    arrive(got)
    piecef = jnp.concatenate([mixed_buf[j].astype(f32) for j in range(nt)], axis=1)
    normed = (piecef * gain).astype(bf16)
    squares = jnp.broadcast_to(jnp.sum(piecef * piecef, axis=1, keepdims=True), (batch, LANES))
    for j in range(nk):
        fsq_part[j] = squares[j * seqs : (j + 1) * seqs]
    got_fsq = exchange("kv", nk, kv, lambda peer: fsq_part.at[peer], fsq_recv.at[kv])
    got_up = []
    for c in range(CHUNKS):
        part = jnp.dot(
            normed, wup_v[:, c * chunk : (c + 1) * chunk], preferred_element_type=f32
        )
        for j in range(nk):
            up_part[c, j] = part[j * seqs : (j + 1) * seqs].astype(bf16)
        got_up.append(
            exchange("kv", nk, kv, lambda peer, c=c: up_part.at[c, peer], up_recv.at[c, kv])
        )
    arrive(got_fsq)
    square_total = total(fsq_part, fsq_recv, kv, nk)
    scale_ffn = lax.rsqrt(square_total[:, :1] / width + EPSILON)
    got_hid = []
    for c in range(CHUNKS):
        arrive(got_up[c])
        up_total = total(up_part.at[c], up_recv.at[c], kv, nk)
        hid_buf[c, kv] = jnp.square(jax.nn.relu(up_total * scale_ffn)).astype(bf16)
        got_hid.append(
            exchange("kv", nk, kv, lambda peer, c=c: hid_buf.at[c, kv], hid_buf.at[c, kv])
        )
    loads["wdown"].wait()
    terms = jnp.zeros((batch, block), f32)
    for c in range(CHUNKS):
        arrive(got_hid[c])
        hidden = stack_rows(hid_buf.at[c], nk).astype(bf16)
        terms = terms + jnp.dot(
            hidden, wdown_v[c * chunk : (c + 1) * chunk, :], preferred_element_type=f32
        )
    for j in range(nt):
        down_part[j] = terms[:, j * cols : (j + 1) * cols].astype(bf16)
    got = exchange("tp", nt, tp, lambda peer: down_part.at[peer], down_recv.at[tp])
    arrive(got_keys)
    arrive(got)
    layer = mixed.astype(f32) + total(down_part, down_recv, tp, nt)
    layer_out[...] = layer.astype(bf16)
    for copy in sent:
        copy.wait_send()


def state_kernel(
    heads,
    head_dim,
    layer,
    rows,
    gates,
    keys,
    cell_state,
    norm_state,
    layer_out,
    cell_next,
    norm_next,
    max_next,
    values_t,
):
    f32 = jnp.float32
    s = pl.program_id(0)
    vrows = rows.shape[2]
    own_heads = vrows // head_dim

    @pl.when(s == 0)
    def _():
        values_t[...] = jnp.transpose(rows[0])
        layer_out[...] = layer[...]
        max_next[...] = gates[0]
        decay = gates[1]
        inflow = gates[2]
        for h in range(heads):
            j, i = divmod(h, own_heads)
            key = keys[j, :, i * head_dim : (i + 1) * head_dim].astype(f32)
            key = key / math.sqrt(head_dim)
            norm_next[:, h, :] = (
                decay[:, h : h + 1] * norm_state[:, h, :] + inflow[:, h : h + 1] * key
            )

    lanes = lax.broadcasted_iota(jnp.int32, values_t.shape, 1)
    column = jnp.sum(jnp.where(lanes == s, values_t[...], 0.0), axis=1, keepdims=True)
    for h in range(own_heads):
        span = slice(h * head_dim, (h + 1) * head_dim)
        gain_k = rows[1, pl.ds(s, 1), span]
        decay = rows[2, pl.ds(s, 1), span]
        cell_next[0, span, :] = decay * cell_state[0, span, :] + column[span] * gain_k


def fused_device(nk, nt, *args):
    f32 = jnp.float32
    bf16 = jnp.bfloat16
    tokens, gain_mix = args[0], args[1]
    w_gates = args[6]
    forget_bias, cell_state, norm_state, max_state = args[7:11]
    w_up = args[14]
    width = gain_mix.shape[0]
    heads = forget_bias.shape[0]
    batch, cols = tokens.shape
    seqs, vrows, head_dim = cell_state.shape
    ffl = w_up.shape[1]
    chunk = ffl // CHUNKS
    block = cols * nt
    vm = pltpu.VMEM
    operands = list(args)
    for i in (1, 7, 11, 13):
        operands[i] = args[i].reshape(1, -1)
    operands[6] = w_gates.T
    landing = [vm(a.shape, a.dtype) for a in operands]
    landing[0] = vm((nt, batch, cols), bf16)
    transfers = (nt - 1) * 6 + (nk - 1) * (7 + 2 * CHUNKS)
    scratch = landing + [
        vm(cell_state.shape, bf16),
        vm((4, nk, seqs, vrows), bf16),
        vm((4, nk, seqs, vrows), bf16),
        vm((nk, seqs, LANES), f32),
        vm((nk, seqs, LANES), f32),
        vm((nk, seqs, vrows), bf16),
        vm((SUBLANES, LANES), f32),
        vm((nt, SUBLANES, LANES), f32),
        vm((nt, batch, cols), bf16),
        vm((nt, batch, cols), bf16),
        vm((nt, batch, cols), bf16),
        vm((nk, seqs, LANES), f32),
        vm((nk, seqs, LANES), f32),
        vm((CHUNKS, nk, seqs, chunk), bf16),
        vm((CHUNKS, nk, seqs, chunk), bf16),
        vm((CHUNKS, nk, seqs, chunk), bf16),
        vm((nt, batch, cols), bf16),
        vm((nt, batch, cols), bf16),
        pltpu.SemaphoreType.DMA((len(operands),)),
        pltpu.SemaphoreType.DMA((transfers,)),
        pltpu.SemaphoreType.DMA((transfers,)),
    ]
    layer, rows, gates, keys = pl.pallas_call(
        functools.partial(fused_kernel, nk, nt, heads, head_dim, width),
        name="fused_step",
        out_shape=(
            jax.ShapeDtypeStruct((batch, cols), bf16),
            jax.ShapeDtypeStruct((3, seqs, vrows), f32),
            jax.ShapeDtypeStruct((3, seqs, heads), f32),
            jax.ShapeDtypeStruct((nt, seqs, vrows), bf16),
        ),
        in_specs=[pl.BlockSpec(memory_space=pl.ANY)] * len(operands),
        out_specs=(pl.BlockSpec(memory_space=pltpu.VMEM),) * 4,
        scratch_shapes=scratch,
        compiler_params=pltpu.CompilerParams(
            collective_id=0, has_side_effects=True, vmem_limit_bytes=56 * 1024 * 1024
        ),
    )(*operands)

    def whole(array):
        zeros = (0,) * len(array.shape)
        return pl.BlockSpec(array.shape, lambda s: zeros)

    step = pl.BlockSpec((1, vrows, head_dim), lambda s: (s, 0, 0))
    layer_out, cell_next, norm_next, max_next = pl.pallas_call(
        functools.partial(state_kernel, heads, head_dim),
        name="state_update",
        grid=(seqs,),
        out_shape=(
            jax.ShapeDtypeStruct((batch, cols), bf16),
            jax.ShapeDtypeStruct(cell_state.shape, f32),
            jax.ShapeDtypeStruct(norm_state.shape, f32),
            jax.ShapeDtypeStruct(max_state.shape, f32),
        ),
        in_specs=[whole(layer), whole(rows), whole(gates), whole(keys), step, whole(norm_state)],
        out_specs=(whole(layer), step, whole(norm_state), whole(max_state)),
        scratch_shapes=[vm((vrows, seqs), f32)],
    )(layer, rows, gates, keys, cell_state, norm_state)
    return layer_out, cell_next, norm_next, max_next


def device_step(nk, nt, *args):
    tokens, cell_state = args[0], args[8]
    batch, cols = tokens.shape
    seqs, vrows, head_dim = cell_state.shape
    ffl = args[14].shape[1]
    fits = (
        cols % LANES == 0
        and vrows % head_dim == 0
        and head_dim % LANES == 0
        and seqs % SUBLANES == 0
        and LANES % (batch // SUBLANES) == 0
        and ffl % (CHUNKS * LANES) == 0
        and 3 * args[7].shape[0] <= LANES
    )
    if fits:
        return fused_device(nk, nt, *args)
    return per_device(*args)


def solution(mesh):
    in_specs = (
        P(None, ("kv", "tp")),
        P(),
        P("kv", "tp"),
        P("kv", "tp"),
        P("kv", "tp"),
        P("kv", "tp"),
        P("kv", None),
        P(),
        P("kv", "tp", None),
        P("kv", None, None),
        P("kv", None),
        P(),
        P("tp", "kv"),
        P(),
        P("kv", "tp"),
        P("tp", "kv"),
    )
    out_specs = (P(None, ("kv", "tp")), P("kv", "tp", None), P("kv", None, None), P("kv", None))
    return jax.shard_map(
        functools.partial(device_step, mesh.shape["kv"], mesh.shape["tp"]),
        mesh=mesh, in_specs=in_specs, out_specs=out_specs, check_vma=False
    )
```

```python
import functools
import math

import jax
import jax.numpy as jnp
from jax import lax
from jax.experimental import pallas as pl
from jax.experimental.pallas import tpu as pltpu
from jax.sharding import PartitionSpec as P

EPSILON = 1e-06


def per_device(
    tokens,
    gain_mix,
    w_query,
    w_key,
    w_value,
    w_outgate,
    w_gates,
    forget_bias,
    cell_state,
    norm_state,
    max_state,
    gain_group,
    w_mix,
    gain_ffn,
    w_up,
    w_down,
):
    f32 = jnp.float32
    bf16 = jnp.bfloat16
    exact = lax.Precision.HIGHEST
    width = gain_mix.shape[0]
    kv_index = lax.axis_index("kv")
    tp_index = lax.axis_index("tp")
    tokf = tokens.astype(f32)
    block_rows = lax.all_gather(tokens, "tp", axis=1, tiled=True)
    block = block_rows.shape[1]
    blockf = block_rows.astype(f32)
    gain_block = lax.dynamic_slice_in_dim(gain_mix, kv_index * block, block)
    normed = (blockf * gain_block).astype(bf16)
    partials = tuple(
        (
            jnp.dot(normed, weight, preferred_element_type=f32)
            for weight in (w_query, w_key, w_value, w_outgate, w_gates)
        )
    )
    partials = partials + (jnp.sum(blockf * blockf, axis=1),)
    summed = lax.psum_scatter(partials, "kv", scatter_dimension=0, tiled=True)
    seqs = summed[0].shape[0]
    seq_squares = summed[5]
    scale_in = lax.rsqrt(seq_squares / width + EPSILON)[:, None]
    query_part = (summed[0] * scale_in).astype(bf16)
    key_part = (summed[1] * scale_in).astype(bf16)
    values = summed[2] * scale_in
    gate_out = summed[3] * scale_in
    gates = summed[4] * scale_in
    query_all, key_all = (
        lax.all_gather(query_part, "tp", axis=1, tiled=True),
        lax.all_gather(key_part, "tp", axis=1, tiled=True),
    )
    heads = forget_bias.shape[0]
    head_dim = cell_state.shape[2]
    value_rows = cell_state.shape[1]
    queryf = query_all.astype(f32).reshape(seqs, heads, head_dim)
    keyf = key_all.astype(f32).reshape(seqs, heads, head_dim) / math.sqrt(head_dim)
    gate_in = gates[:, :heads]
    log_forget = jax.nn.log_sigmoid(gates[:, heads:] + forget_bias)
    max_next = jnp.maximum(log_forget + max_state, gate_in)
    decay = jnp.exp(log_forget + max_state - max_next)
    inflow = jnp.exp(gate_in - max_next)
    norm_next = decay[..., None] * norm_state + inflow[..., None] * keyf
    denom_heads = jnp.maximum(jnp.abs(jnp.sum(norm_next * queryf, axis=2)), 1.0)
    row_ids = tp_index * value_rows + jnp.arange(value_rows)
    select = (row_ids[:, None] // head_dim == jnp.arange(heads)[None, :]).astype(f32)
    query_rows = jnp.einsum("shd,rh->srd", queryf, select, precision=exact)
    key_rows = jnp.einsum("shd,rh->srd", keyf, select, precision=exact)
    decay_rows = jnp.einsum("sh,rh->sr", decay, select, precision=exact)
    inflow_rows = jnp.einsum("sh,rh->sr", inflow, select, precision=exact)
    denom_rows = jnp.einsum("sh,rh->sr", denom_heads, select, precision=exact)
    cell_next = (
        decay_rows[:, :, None] * cell_state
        + inflow_rows[:, :, None] * values[:, :, None] * key_rows
    )
    numer = jnp.sum(cell_next * query_rows, axis=2)
    cell_read = (jax.nn.sigmoid(gate_out) * (numer / denom_rows)).astype(bf16)
    read_rows = lax.all_gather(cell_read, "kv", axis=0, tiled=True)
    readf = read_rows.astype(f32)
    group_total = lax.psum(jnp.sum(readf * readf, axis=1), "tp")
    scale_group = lax.rsqrt(group_total / (heads * head_dim) + EPSILON)[:, None]
    gain_rows = lax.dynamic_slice_in_dim(gain_group, tp_index * value_rows, value_rows)
    grouped = (readf * gain_rows).astype(bf16)
    mix_terms = jnp.dot(grouped, w_mix, preferred_element_type=f32)
    mix_summed = lax.psum_scatter(mix_terms, "tp", scatter_dimension=1, tiled=True)
    mixed = (tokf + mix_summed * scale_group).astype(bf16)
    ffn_block = w_up.shape[0]
    piece = lax.all_gather(mixed, "tp", axis=1, tiled=True)
    count = piece.shape[1]
    piecef = piece.astype(f32)
    gain_piece = lax.dynamic_slice_in_dim(gain_ffn, kv_index * ffn_block, count)
    normed_piece = (piecef * gain_piece).astype(bf16)
    up_part = jnp.dot(normed_piece, w_up, preferred_element_type=f32)
    square_part = jnp.sum(piecef * piecef, axis=1)
    up_total, square_total = lax.psum((up_part, square_part), "kv")
    scale_ffn = lax.rsqrt(square_total / width + EPSILON)[:, None]
    hidden = jnp.square(jax.nn.relu(up_total * scale_ffn)).astype(bf16)
    down_terms = jnp.dot(hidden, w_down, preferred_element_type=f32)
    ffn_summed = lax.psum_scatter(down_terms, "tp", scatter_dimension=1, tiled=True)
    layer_out = (mixed.astype(f32) + ffn_summed).astype(bf16)
    return (layer_out, cell_next, norm_next, max_next)


MESH = pl.DeviceIdType.MESH
LANES = 128
SUBLANES = 8
CHUNKS = 2
VMEM_BYTES = 67043328


def stack_rows(ref, count):
    f32 = jnp.float32
    rows = [ref[j].astype(f32) for j in range(count)]
    return jnp.concatenate(rows, axis=0)


def fused_kernel(
    nk,
    nt,
    heads,
    head_dim,
    width,
    tokens,
    gain_mix,
    w_query,
    w_key,
    w_value,
    w_outgate,
    w_gates,
    forget_bias,
    cell_state,
    norm_state,
    max_state,
    gain_group,
    w_mix,
    gain_ffn,
    w_up,
    w_down,
    layer_out,
    cell_out,
    norm_out,
    max_out,
    keys_buf,
    tok_v,
    gmix_v,
    wq_v,
    wk_v,
    wv_v,
    wo_v,
    wg_v,
    bias_v,
    cell_v,
    norm_v,
    max_v,
    ggroup_v,
    wmix_v,
    gffn_v,
    wup_v,
    wdown_v,
    cell_b,
    proj_part,
    proj_recv,
    gate_part,
    gate_recv,
    read_buf,
    sq_part,
    sq_recv,
    mix_part,
    mix_recv,
    mixed_buf,
    fsq_part,
    fsq_recv,
    up_part,
    up_recv,
    hid_buf,
    down_part,
    down_recv,
    local_sem,
    send_sem,
    recv_sem,
):
    f32 = jnp.float32
    bf16 = jnp.bfloat16
    kv = lax.axis_index("kv")
    tp = lax.axis_index("tp")
    batch, cols = tokens.shape
    seqs = batch // nk
    block = cols * nt
    vrows = wq_v.shape[1]
    own_heads = vrows // head_dim
    ffl = wup_v.shape[1]
    chunk = ffl // CHUNKS

    loads = {}

    def load(name, source, target):
        copy = pltpu.make_async_copy(source, target, local_sem.at[len(loads)])
        copy.start()
        loads[name] = copy

    load("tok", tokens, tok_v.at[tp])
    load("gmix", gain_mix, gmix_v)
    load("wq", w_query, wq_v)
    load("wk", w_key, wk_v)
    load("wv", w_value, wv_v)
    load("wo", w_outgate, wo_v)
    load("wg", w_gates, wg_v)

    barrier = pltpu.get_barrier_semaphore()
    for d in range(1, nt):
        pl.semaphore_signal(
            barrier, inc=1, device_id={"tp": lax.rem(tp + d, nt)}, device_id_type=MESH
        )
    for d in range(1, nk):
        pl.semaphore_signal(
            barrier, inc=1, device_id={"kv": lax.rem(kv + d, nk)}, device_id_type=MESH
        )
    pl.semaphore_wait(barrier, nt + nk - 2)

    used = [0]
    sent = []

    def exchange(axis, count, me, source, target):
        copies = []
        for d in range(1, count):
            peer = lax.rem(me + d, count)
            copy = pltpu.make_async_remote_copy(
                src_ref=source(peer),
                dst_ref=target,
                send_sem=send_sem.at[used[0]],
                recv_sem=recv_sem.at[used[0]],
                device_id={axis: peer},
                device_id_type=MESH,
            )
            copy.start()
            used[0] += 1
            copies.append(copy)
        sent.extend(copies)
        return copies

    def arrive(copies):
        for copy in copies:
            copy.wait_recv()

    def total(own, recv, me, count):
        result = own[me].astype(f32)
        for d in range(1, count):
            result = result + recv[lax.rem(me + count - d, count)].astype(f32)
        return result

    got = exchange("tp", nt, tp, lambda peer: tokens, tok_v.at[tp])
    load("cell", cell_state, cell_v)
    load("norm", norm_state, norm_v)
    load("max", max_state, max_v)
    load("bias", forget_bias, bias_v)
    load("ggroup", gain_group, ggroup_v)
    load("gffn", gain_ffn, gffn_v)
    load("wmix", w_mix, wmix_v)
    load("wup", w_up, wup_v)
    load("wdown", w_down, wdown_v)
    loads["tok"].wait()
    loads["gmix"].wait()
    arrive(got)
    blockf = jnp.concatenate([tok_v[j].astype(f32) for j in range(nt)], axis=1)
    gain = gmix_v[:, pl.ds(pl.multiple_of(kv * block, LANES), block)]
    normed = (blockf * gain).astype(bf16)
    squares = jnp.sum(blockf * blockf, axis=1, keepdims=True)
    loads["wg"].wait()
    gates_p = lax.dot_general(
        normed, wg_v[...], (((1,), (1,)), ((), ())), preferred_element_type=f32
    )
    squares_b = jnp.broadcast_to(squares, (batch, LANES))
    for j in range(nk):
        gate_part[j] = squares_b[j * seqs : (j + 1) * seqs]
        gate_part[j, :, : 2 * heads] = gates_p[j * seqs : (j + 1) * seqs]
    got_gates = exchange("kv", nk, kv, lambda peer: gate_part.at[peer], gate_recv.at[kv])
    got_proj = []
    for i, (name, weight) in enumerate((("wq", wq_v), ("wk", wk_v), ("wv", wv_v), ("wo", wo_v))):
        loads[name].wait()
        part = jnp.dot(normed, weight[...], preferred_element_type=f32)
        for j in range(nk):
            proj_part[i, j] = part[j * seqs : (j + 1) * seqs].astype(bf16)
        got_proj.append(
            exchange("kv", nk, kv, lambda peer, i=i: proj_part.at[i, peer], proj_recv.at[i, kv])
        )

    loads["cell"].wait()
    for s in range(seqs):
        cell_b[s] = cell_v[s].astype(bf16)
    loads["norm"].wait()
    loads["max"].wait()
    loads["bias"].wait()

    arrive(got_gates)
    gsum = total(gate_part, gate_recv, kv, nk)
    scale_in = lax.rsqrt(gsum[:, 2 * heads : 2 * heads + 1] / width + EPSILON)
    scaled = gsum * scale_in
    gate_in = scaled[:, :heads]
    gate_forget = pltpu.roll(scaled, LANES - heads, 1)[:, :heads]
    max_state_ = max_v[...]
    log_forget = jax.nn.log_sigmoid(gate_forget + bias_v[...])
    max_next = jnp.maximum(log_forget + max_state_, gate_in)
    decay = jnp.exp(log_forget + max_state_ - max_next)
    inflow = jnp.exp(gate_in - max_next)
    max_out[...] = max_next
    head_ids = lax.broadcasted_iota(jnp.int32, (seqs, heads), 1)

    def own(values, h):
        mine = jnp.where(head_ids == tp * own_heads + h, values, 0.0)
        return jnp.sum(mine, axis=1, keepdims=True)

    own_decay = [own(decay, h) for h in range(own_heads)]
    own_inflow = [own(inflow, h) for h in range(own_heads)]
    norm_ids = lax.broadcasted_iota(jnp.int32, (seqs, heads, head_dim), 1)
    norm_own = [
        jnp.sum(jnp.where(norm_ids == tp * own_heads + h, norm_v[...], 0.0), axis=1)
        for h in range(own_heads)
    ]

    sums = []
    for i in range(4):
        arrive(got_proj[i])
        sums.append(total(proj_part.at[i], proj_recv.at[i], kv, nk) * scale_in)
    query = sums[0].astype(bf16)
    key = sums[1].astype(bf16)
    values = sums[2]
    opened = jax.nn.sigmoid(sums[3])
    keys_buf[tp] = key
    queryf = query.astype(f32)
    keyf = key.astype(f32) / math.sqrt(head_dim)
    row_ids = lax.broadcasted_iota(jnp.int32, (seqs, head_dim), 0)
    reads = []
    gain_keys = []
    for h in range(own_heads):
        span = slice(h * head_dim, (h + 1) * head_dim)
        qh = queryf[:, span]
        kh = keyf[:, span]
        numer = jnp.zeros((seqs, head_dim), f32)
        for s in range(seqs):
            lhs = jnp.where(row_ids == s, qh, 0.0).astype(bf16)
            numer += lax.dot_general(
                lhs,
                cell_b[s, span, :],
                (((1,), (1,)), ((), ())),
                preferred_element_type=f32,
            )
        gain_k = own_inflow[h] * kh
        norm_h = own_decay[h] * norm_own[h] + gain_k
        denom = jnp.maximum(jnp.abs(jnp.sum(norm_h * qh, axis=1, keepdims=True)), 1.0)
        kq = jnp.sum(gain_k * qh, axis=1, keepdims=True)
        numer = own_decay[h] * numer + values[:, span] * kq
        reads.append((opened[:, span] * (numer / denom)).astype(bf16))
        gain_keys.append(gain_k)
    read_buf[kv] = jnp.concatenate(reads, axis=1)
    got = exchange("kv", nk, kv, lambda peer: read_buf.at[kv], read_buf.at[kv])
    got_keys = exchange("tp", nt, tp, lambda peer: keys_buf.at[tp], keys_buf.at[tp])
    values_t = jnp.transpose(values)

    def update(first, last):
        for s in range(first, last):
            for h in range(own_heads):
                span = slice(h * head_dim, (h + 1) * head_dim)
                cell_out[s, span, :] = (
                    own_decay[h][s : s + 1] * cell_v[s, span, :]
                    + values_t[span, s : s + 1] * gain_keys[h][s : s + 1]
                )

    third = seqs // 3
    update(0, third)
    loads["ggroup"].wait()
    loads["wmix"].wait()
    gain = ggroup_v[:, pl.ds(pl.multiple_of(tp * vrows, LANES), vrows)]
    arrive(got)
    readf = stack_rows(read_buf, nk)
    groups = batch // SUBLANES
    stride = LANES // groups
    squares = jnp.sum(readf * readf, axis=1, keepdims=True)
    lane_ids = lax.broadcasted_iota(jnp.int32, (SUBLANES, LANES), 1)
    packed = jnp.zeros((SUBLANES, LANES), f32)
    for a in range(groups):
        packed = jnp.where(
            lane_ids // stride == a, squares[a * SUBLANES : (a + 1) * SUBLANES], packed
        )
    sq_part[...] = packed
    got_sq = exchange("tp", nt, tp, lambda peer: sq_part, sq_recv.at[tp])
    grouped = (readf * gain).astype(bf16)
    terms = jnp.dot(grouped, wmix_v[...], preferred_element_type=f32)
    for j in range(nt):
        mix_part[j] = terms[:, j * cols : (j + 1) * cols].astype(bf16)
    got = exchange("tp", nt, tp, lambda peer: mix_part.at[peer], mix_recv.at[tp])
    tokf = tok_v[tp].astype(f32)
    update(third, 2 * third)
    arrive(got_sq)
    for d in range(1, nt):
        packed = packed + sq_recv[lax.rem(tp + nt - d, nt)]
    scale_packed = lax.rsqrt(packed / (heads * head_dim) + EPSILON)
    scale_group = jnp.concatenate(
        [scale_packed[:, a * stride : a * stride + 1] for a in range(groups)], axis=0
    )
    arrive(got)
    mixed = (tokf + total(mix_part, mix_recv, tp, nt) * scale_group).astype(bf16)
    mixed_buf[tp] = mixed
    got = exchange("tp", nt, tp, lambda peer: mixed_buf.at[tp], mixed_buf.at[tp])
    update(2 * third, seqs)
    loads["gffn"].wait()
    loads["wup"].wait()
    gain = gffn_v[:, pl.ds(pl.multiple_of(kv * block, LANES), block)]
    arrive(got)
    piecef = jnp.concatenate([mixed_buf[j].astype(f32) for j in range(nt)], axis=1)
    normed = (piecef * gain).astype(bf16)
    squares = jnp.broadcast_to(jnp.sum(piecef * piecef, axis=1, keepdims=True), (batch, LANES))
    for j in range(nk):
        fsq_part[j] = squares[j * seqs : (j + 1) * seqs]
    got_fsq = exchange("kv", nk, kv, lambda peer: fsq_part.at[peer], fsq_recv.at[kv])
    got_up = []
    for c in range(CHUNKS):
        part = jnp.dot(
            normed, wup_v[:, c * chunk : (c + 1) * chunk], preferred_element_type=f32
        )
        for j in range(nk):
            up_part[c, j] = part[j * seqs : (j + 1) * seqs].astype(bf16)
        got_up.append(
            exchange("kv", nk, kv, lambda peer, c=c: up_part.at[c, peer], up_recv.at[c, kv])
        )
    arrive(got_fsq)
    square_total = total(fsq_part, fsq_recv, kv, nk)
    scale_ffn = lax.rsqrt(square_total[:, :1] / width + EPSILON)
    got_hid = []
    for c in range(CHUNKS):
        arrive(got_up[c])
        up_total = total(up_part.at[c], up_recv.at[c], kv, nk)
        hid_buf[c, kv] = jnp.square(jax.nn.relu(up_total * scale_ffn)).astype(bf16)
        got_hid.append(
            exchange("kv", nk, kv, lambda peer, c=c: hid_buf.at[c, kv], hid_buf.at[c, kv])
        )
    loads["wdown"].wait()
    terms = jnp.zeros((batch, block), f32)
    for c in range(CHUNKS):
        arrive(got_hid[c])
        hidden = stack_rows(hid_buf.at[c], nk).astype(bf16)
        terms = terms + jnp.dot(
            hidden, wdown_v[c * chunk : (c + 1) * chunk, :], preferred_element_type=f32
        )
    for j in range(nt):
        down_part[j] = terms[:, j * cols : (j + 1) * cols].astype(bf16)
    got = exchange("tp", nt, tp, lambda peer: down_part.at[peer], down_recv.at[tp])
    arrive(got_keys)
    for h in range(heads):
        j, i = divmod(h, own_heads)
        key = keys_buf[j, :, i * head_dim : (i + 1) * head_dim].astype(f32)
        key = key / math.sqrt(head_dim)
        norm_out[:, h, :] = decay[:, h : h + 1] * norm_v[:, h, :] + inflow[:, h : h + 1] * key
    arrive(got)
    layer = mixed.astype(f32) + total(down_part, down_recv, tp, nt)
    layer_out[...] = layer.astype(bf16)
    for copy in sent:
        copy.wait_send()


def store_kernel(layer, cell, norm, top, layer_out, cell_out, norm_out, max_out, sems):
    seqs = cell.shape[0]
    copies = [(cell.at[s], cell_out.at[s]) for s in range(seqs)]
    copies += [(layer, layer_out), (norm, norm_out), (top, max_out)]
    copies = [pltpu.make_async_copy(a, b, sems.at[i]) for i, (a, b) in enumerate(copies)]
    for copy in copies:
        copy.start()
    for copy in copies:
        copy.wait()


def fused_device(nk, nt, *args):
    f32 = jnp.float32
    bf16 = jnp.bfloat16
    tokens, gain_mix = args[0], args[1]
    w_gates = args[6]
    forget_bias, cell_state, norm_state, max_state = args[7:11]
    w_up = args[14]
    width = gain_mix.shape[0]
    heads = forget_bias.shape[0]
    batch, cols = tokens.shape
    seqs, vrows, head_dim = cell_state.shape
    ffl = w_up.shape[1]
    chunk = ffl // CHUNKS
    block = cols * nt
    vm = pltpu.VMEM
    operands = list(args)
    for i in (1, 7, 11, 13):
        operands[i] = args[i].reshape(1, -1)
    operands[6] = w_gates.T
    landing = [vm(a.shape, a.dtype) for a in operands]
    landing[0] = vm((nt, batch, cols), bf16)
    transfers = (nt - 1) * 6 + (nk - 1) * (7 + 2 * CHUNKS)
    scratch = landing + [
        vm(cell_state.shape, bf16),
        vm((4, nk, seqs, vrows), bf16),
        vm((4, nk, seqs, vrows), bf16),
        vm((nk, seqs, LANES), f32),
        vm((nk, seqs, LANES), f32),
        vm((nk, seqs, vrows), bf16),
        vm((SUBLANES, LANES), f32),
        vm((nt, SUBLANES, LANES), f32),
        vm((nt, batch, cols), bf16),
        vm((nt, batch, cols), bf16),
        vm((nt, batch, cols), bf16),
        vm((nk, seqs, LANES), f32),
        vm((nk, seqs, LANES), f32),
        vm((CHUNKS, nk, seqs, chunk), bf16),
        vm((CHUNKS, nk, seqs, chunk), bf16),
        vm((CHUNKS, nk, seqs, chunk), bf16),
        vm((nt, batch, cols), bf16),
        vm((nt, batch, cols), bf16),
        pltpu.SemaphoreType.DMA((len(operands),)),
        pltpu.SemaphoreType.DMA((transfers,)),
        pltpu.SemaphoreType.DMA((transfers,)),
    ]
    results = (
        ((batch, cols), bf16),
        (cell_state.shape, f32),
        (norm_state.shape, f32),
        (max_state.shape, f32),
    )
    kept = 4 * batch * cols + 4 * cell_state.size + 4 * norm_state.size + 2**16
    held = pl.pallas_call(
        functools.partial(fused_kernel, nk, nt, heads, head_dim, width),
        name="fused_step",
        out_shape=tuple(vm(shape, dtype) for shape, dtype in results),
        in_specs=[pl.BlockSpec(memory_space=pltpu.HBM)] * len(operands),
        out_specs=(pl.BlockSpec(memory_space=pltpu.VMEM),) * 4,
        scratch_shapes=[vm((nt, seqs, vrows), bf16)] + scratch,
        compiler_params=pltpu.CompilerParams(
            collective_id=0, has_side_effects=True, vmem_limit_bytes=VMEM_BYTES - kept
        ),
    )(*operands)
    return pl.pallas_call(
        store_kernel,
        name="store_results",
        out_shape=tuple(jax.ShapeDtypeStruct(shape, dtype) for shape, dtype in results),
        in_specs=[pl.BlockSpec(memory_space=pltpu.VMEM)] * 4,
        out_specs=(pl.BlockSpec(memory_space=pl.ANY),) * 4,
        scratch_shapes=[pltpu.SemaphoreType.DMA((seqs + 3,))],
        compiler_params=pltpu.CompilerParams(vmem_limit_bytes=16 * 1024 * 1024),
    )(*held)


def device_step(nk, nt, *args):
    tokens, cell_state = args[0], args[8]
    batch, cols = tokens.shape
    seqs, vrows, head_dim = cell_state.shape
    ffl = args[14].shape[1]
    fits = (
        cols % LANES == 0
        and vrows % head_dim == 0
        and head_dim % LANES == 0
        and seqs % SUBLANES == 0
        and LANES % (batch // SUBLANES) == 0
        and ffl % (CHUNKS * LANES) == 0
        and 3 * args[7].shape[0] <= LANES
    )
    if fits:
        return fused_device(nk, nt, *args)
    return per_device(*args)


def solution(mesh):
    in_specs = (
        P(None, ("kv", "tp")),
        P(),
        P("kv", "tp"),
        P("kv", "tp"),
        P("kv", "tp"),
        P("kv", "tp"),
        P("kv", None),
        P(),
        P("kv", "tp", None),
        P("kv", None, None),
        P("kv", None),
        P(),
        P("tp", "kv"),
        P(),
        P("kv", "tp"),
        P("tp", "kv"),
    )
    out_specs = (P(None, ("kv", "tp")), P("kv", "tp", None), P("kv", None, None), P("kv", None))
    return jax.shard_map(
        functools.partial(device_step, mesh.shape["kv"], mesh.shape["tp"]),
        mesh=mesh, in_specs=in_specs, out_specs=out_specs, check_vma=False
    )
```
